32 devices in a mesh: kv: 16 (over z, y, core), tp: 2 (over x).
Axes of the slice: x: 2, y: 2, z: 4, core: 2. Of those that a mesh axis runs over, the one named last changes fastest.
Arguments:
- hidden_in: bfloat16 [32, 3072], replicated, may hold values from -60 to 60
- in_gain: bfloat16 [3072], replicated, may hold values from 0.099609375 to 1.8984375
- query_weight: bfloat16 [3072, 1536], P(None, 'tp'), may hold values from -0.109375 to 0.109375
- key_weight: bfloat16 [3072, 256], replicated, may hold values from -0.109375 to 0.109375
- value_weight: bfloat16 [3072, 256], replicated, may hold values from -0.109375 to 0.109375
- key_cache: bfloat16 [32, 2, 1024, 128], P(None, None, 'kv'), may hold values from -200 to 200
- value_cache: bfloat16 [32, 2, 1024, 128], P(None, None, 'kv'), may hold values from -6 to 6
- lengths: int32 [32], replicated, may hold values from 256 to 1023
- mix_lambda: float32 [12], P('tp'), may hold values from 0.3 to 0.8
- head_gain: bfloat16 [12, 128], P('tp'), may hold values from 0.099609375 to 1.8984375
- out_weight: bfloat16 [1536, 3072], P('tp', 'kv'), may hold values from -0.15625 to 0.15625
Outputs:
- mixed: bfloat16 [32, 3072], P(None, 'kv')
- new_keys: bfloat16 [32, 2, 128], replicated
- new_values: bfloat16 [32, 2, 128], replicated
The draws below stay inside these ranges and needn't reach their ends.
All inputs are finite; a program needn't handle non-finite values.
Results may differ from the reference program's by a relative error of at most 0.013.
The reference program's roundings to bfloat16 on the way count: a program that leaves them out, or rounds other values in their place, can miss the bound.
Values may be sent and summed in bfloat16 or wider, within the bound.
A program may use at most 64 MiB of HBM per device.

```python
import math
import jax
import jax.numpy as jnp
from jax import lax

D = 3072
HEADS = 12
KV_HEADS = 2
HEAD_DIM = 64
VALUE_DIM = 128
SEQS = 32
POS_DEV = 64
CACHE_LEN = 1024
N_KV = 16
N_TP = 2


def draw_hidden_in(key, part):
    noise_key = jax.random.fold_in(jax.random.fold_in(key, 3), 0)
    column_ramp = jnp.exp(jnp.linspace(jnp.log(0.5), jnp.log(1.5), D))
    values = jnp.clip(jax.random.normal(noise_key, (SEQS, D), jnp.float32), -5.0, 5.0) * column_ramp[None, :]
    return values.astype(jnp.bfloat16)


def draw_key_cache(key, part):
    base_key = jax.random.fold_in(jax.random.fold_in(key, 11), 0)
    shape = (SEQS, KV_HEADS, CACHE_LEN, 2 * HEAD_DIM)
    values = jnp.clip(jax.random.normal(base_key, shape, jnp.float32), -4.0, 4.0) * 1.75
    return values.astype(jnp.bfloat16)


def plant(array, own_key, low, largest):
    dims = array.shape
    spot = [jax.random.randint(jax.random.fold_in(own_key, axis), (), 0, dims[axis]) for axis in range(len(dims))]
    array = array.at[tuple(spot)].set(low)
    longest = dims.index(max(dims))
    spot[longest] = (spot[longest] + 1) % dims[longest]
    return array.at[tuple(spot)].set(largest)


def shard_levels(rng, dims, pieces, smallest, largest):
    loudness, own = 1.0, jax.random.fold_in(rng, 6)
    for dim, shards_of in pieces:
        steps = jnp.exp(jax.random.uniform(jax.random.fold_in(own, dim), (shards_of,), jnp.float32, smallest / len(pieces), largest / len(pieces)))
        loudness = loudness * jnp.repeat(steps, dims[dim] // shards_of).reshape([-1 if axis == dim else 1 for axis in range(len(dims))])
    return loudness


def centred(own_key, dims, spread, most, pieces=(), held_as=jnp.bfloat16):
    loudness = shard_levels(own_key, dims, pieces, -0.22, 0.18) if pieces else 1.0
    values = jax.random.normal(own_key, dims, jnp.float32) * spread * loudness
    return jnp.minimum(jnp.maximum(values, -most), most).astype(held_as)


def setup_inputs(seed: int = 0) -> dict:
    key_of = jax.random.split(jax.random.key(seed), 12)
    hidden_in = draw_hidden_in(jax.random.fold_in(key_of[11], 71), 0)
    in_gain = jnp.clip(1.0 + 0.18 * jax.random.normal(key_of[1], (D,), jnp.float32), 0.099609375, 1.8984375).astype(jnp.bfloat16)
    query_weight = centred(key_of[2], (D, HEADS * 2 * HEAD_DIM), D ** -0.5, 0.109375, ((1, 2),))
    key_weight = centred(key_of[3], (D, KV_HEADS * 2 * HEAD_DIM), D ** -0.5, 0.109375)
    value_weight = centred(key_of[4], (D, KV_HEADS * VALUE_DIM), D ** -0.5, 0.109375)
    key_cache = draw_key_cache(jax.random.fold_in(key_of[11], 71), 0)
    value_cache = centred(key_of[6], (SEQS, KV_HEADS, CACHE_LEN, VALUE_DIM), 1.0, 6.0, ((2, 16),))
    lengths = plant(jax.random.randint(key_of[7], (SEQS,), CACHE_LEN // 4, CACHE_LEN), jax.random.fold_in(key_of[7], 1), CACHE_LEN // 4, CACHE_LEN - 1).astype(jnp.int32)
    mix_lambda = jnp.clip(0.3 + 0.5 * jax.random.uniform(key_of[8], (HEADS,), jnp.float32) ** shard_levels(key_of[8], (HEADS,), ((0, 2),), -0.2, 0.2), 0.3, 0.8)
    head_gain = jnp.clip(1.0 + 0.18 * jax.random.normal(key_of[9], (HEADS, VALUE_DIM), jnp.float32), 0.099609375, 1.8984375).astype(jnp.bfloat16)
    out_weight = centred(key_of[10], (HEADS * VALUE_DIM, D), (HEADS * VALUE_DIM) ** -0.5, 0.15625, ((0, 2), (1, 16)))
    return dict(hidden_in=hidden_in, in_gain=in_gain, query_weight=query_weight, key_weight=key_weight, value_weight=value_weight, key_cache=key_cache, value_cache=value_cache, lengths=lengths, mix_lambda=mix_lambda, head_gain=head_gain, out_weight=out_weight)


EPS = 1e-06
THETA = 500000.0
NEG = -1e+30

def rotate(vectors, position):
    half_dim = vectors.shape[-1] // 2
    frequency = THETA ** (-jnp.arange(half_dim, dtype=jnp.float32) * 2.0 / vectors.shape[-1])
    angles = position[:, None, None, None] * frequency
    cosine = jnp.cos(angles)
    sine_part = jnp.sin(angles)
    lower_half = vectors[..., :half_dim]
    upper_half = vectors[..., half_dim:]
    return jnp.concatenate([lower_half * cosine - upper_half * sine_part, upper_half * cosine + lower_half * sine_part], axis=-1)

def reference(hidden_in, in_gain, query_weight, key_weight, value_weight, key_cache, value_cache, lengths, mix_lambda, head_gain, out_weight):
    inputs = hidden_in.astype(jnp.float32)
    inverse = lax.rsqrt(lax.optimization_barrier(jnp.mean(inputs * inputs, axis=-1, keepdims=True)) + EPS)
    scaled = (inputs * in_gain.astype(jnp.float32)).astype(jnp.bfloat16)
    position = lengths.astype(jnp.float32)
    queries = rotate((jnp.dot(scaled, query_weight, preferred_element_type=jnp.float32) * inverse).reshape(SEQS, HEADS, 2, HEAD_DIM), position).astype(jnp.bfloat16)
    new_keys = rotate((jnp.dot(scaled, key_weight, preferred_element_type=jnp.float32) * inverse).reshape(SEQS, KV_HEADS, 2, HEAD_DIM), position).astype(jnp.bfloat16)
    new_values = (jnp.dot(scaled, value_weight, preferred_element_type=jnp.float32) * inverse).astype(jnp.bfloat16).reshape(SEQS, KV_HEADS, VALUE_DIM)
    group_size = HEADS // KV_HEADS
    grouped = queries.reshape(SEQS, KV_HEADS, group_size, 2, HEAD_DIM).astype(jnp.float32)
    scale_root = math.sqrt(HEAD_DIM)

    def combine(state_tuple, block_index):
        running_max, running_sum, weighted = state_tuple
        block_start = (block_index * POS_DEV).astype(jnp.int32)
        block_keys = lax.dynamic_slice_in_dim(key_cache, block_start, POS_DEV, 2).reshape(SEQS, KV_HEADS, POS_DEV, 2, HEAD_DIM).astype(jnp.float32)
        block_values = lax.dynamic_slice_in_dim(value_cache, block_start, POS_DEV, 2).astype(jnp.float32)
        scores = jnp.einsum('bgmcd,bgpcd->bgmcp', grouped, block_keys) / scale_root
        places = block_start + jnp.arange(POS_DEV, dtype=jnp.int32)
        visible = (places[None, :] < lengths[:, None])[:, None, None, None, :]
        scores = jnp.where(visible, scores, NEG)
        local_max = lax.optimization_barrier(jnp.max(scores, axis=-1))
        weights = jnp.where(visible, jnp.exp(scores - local_max[..., None]), 0.0)
        local_sum = lax.optimization_barrier(jnp.sum(weights, axis=-1))
        rounded = weights.astype(jnp.bfloat16).astype(jnp.float32)
        local_values = jnp.einsum('bgmcp,bgpe->bgmce', rounded, block_values)
        joint = jnp.maximum(running_max, local_max)
        old_factor = jnp.exp(running_max - joint)
        new_factor = jnp.exp(local_max - joint)
        return ((joint, running_sum * old_factor + local_sum * new_factor, weighted * old_factor[..., None] + local_values * new_factor[..., None]), None)
    start_max = jnp.full((SEQS, KV_HEADS, group_size, 2), NEG, jnp.float32)
    start_sum = jnp.zeros((SEQS, KV_HEADS, group_size, 2), jnp.float32)
    start_values = jnp.zeros((SEQS, KV_HEADS, group_size, 2, VALUE_DIM), jnp.float32)
    state_tuple, unused = lax.scan(combine, (start_max, start_sum, start_values), jnp.arange(N_KV, dtype=jnp.int32))
    running_max, running_sum, weighted = state_tuple
    own_scores = jnp.einsum('bgmcd,bgcd->bgmc', grouped, new_keys.astype(jnp.float32)) / scale_root
    joint = jnp.maximum(running_max, own_scores)
    past_factor = jnp.exp(running_max - joint)
    own_weight = jnp.exp(own_scores - joint)
    running_sum = running_sum * past_factor + own_weight
    weighted = weighted * past_factor[..., None] + own_weight[..., None] * new_values.astype(jnp.float32)[:, :, None, None, :]
    outputs = weighted / running_sum[..., None]
    lambda_rows = mix_lambda.reshape(KV_HEADS, group_size)[None, :, :, None]
    head_out = (outputs[..., 0, :] - lambda_rows * outputs[..., 1, :]).reshape(SEQS, HEADS, VALUE_DIM)
    normed = (head_out * lax.rsqrt(lax.optimization_barrier(jnp.mean(head_out * head_out, axis=-1, keepdims=True)) + EPS) * head_gain.astype(jnp.float32)).astype(jnp.bfloat16)
    per_group = normed.reshape(SEQS, N_TP, HEADS // N_TP * VALUE_DIM).astype(jnp.float32)
    weight_groups = out_weight.reshape(N_TP, HEADS // N_TP * VALUE_DIM, D).astype(jnp.float32)
    partials = jnp.einsum('bti,tid->tbd', per_group, weight_groups).astype(jnp.bfloat16)
    partials = lax.optimization_barrier(partials).astype(jnp.float32)
    mixed = lax.optimization_barrier(jnp.sum(partials, axis=0)).astype(jnp.bfloat16)
    return (mixed, new_keys.reshape(SEQS, KV_HEADS, 2 * HEAD_DIM), new_values)
```

```python
import functools
import math

import jax
import jax.numpy as jnp
import numpy as np
from jax import lax
from jax.experimental import pallas as pl
from jax.experimental.pallas import tpu as pltpu
from jax.sharding import PartitionSpec as P

HEADS = 12
KV_HEADS = 2


EPS = 1e-06
THETA = 500000.0
NEG = -1e30


def joined(value, axis, join):
    pieces = jax.tree.map(lambda part: lax.all_gather(part, axis), value)
    head = jax.tree.map(lambda part: part[0], pieces)
    tail = jax.tree.map(lambda part: part[1:], pieces)
    subtotal, _ = lax.scan(lambda subtotal, section: (join(subtotal, section), None), head, tail)
    return subtotal


def rotate(vectors, position):
    half_dim = vectors.shape[-1] // 2
    frequency = THETA ** (-jnp.arange(half_dim, dtype=jnp.float32) * 2.0 / vectors.shape[-1])
    angles = position[:, None, None, None] * frequency
    cosine = jnp.cos(angles)
    sine_part = jnp.sin(angles)
    lower_half = vectors[..., :half_dim]
    upper_half = vectors[..., half_dim:]
    return jnp.concatenate(
        [
            lower_half * cosine - upper_half * sine_part,
            upper_half * cosine + lower_half * sine_part,
        ],
        axis=-1,
    )


def merge_parts(earlier, later):
    max_early, sum_early, values_early = earlier
    max_late, sum_late, values_late = later
    joint = jnp.maximum(max_early, max_late)
    early_factor = jnp.exp(max_early - joint)
    late_factor = jnp.exp(max_late - joint)
    return (
        joint,
        sum_early * early_factor + sum_late * late_factor,
        values_early * early_factor[..., None] + values_late * late_factor[..., None],
    )


def per_device(
    hidden_in,
    in_gain,
    query_weight,
    key_weight,
    value_weight,
    key_cache,
    value_cache,
    lengths,
    mix_lambda,
    head_gain,
    out_weight,
):
    seq_count = hidden_in.shape[0]
    local_heads = mix_lambda.shape[0]
    head_dim = query_weight.shape[1] // (2 * local_heads)
    kv_count = key_cache.shape[1]
    span_len = key_cache.shape[2]
    value_dim = value_cache.shape[3]
    inputs = hidden_in.astype(jnp.float32)
    inverse = lax.rsqrt(jnp.mean(inputs * inputs, axis=-1, keepdims=True) + EPS)
    scaled = (inputs * in_gain.astype(jnp.float32)).astype(jnp.bfloat16)
    position = lengths.astype(jnp.float32)
    query_part = jnp.dot(scaled, query_weight, preferred_element_type=jnp.float32)
    key_part = jnp.dot(scaled, key_weight, preferred_element_type=jnp.float32)
    value_part = jnp.dot(scaled, value_weight, preferred_element_type=jnp.float32)
    queries = rotate(
        (query_part * inverse).reshape(seq_count, local_heads, 2, head_dim), position
    ).astype(jnp.bfloat16)
    new_keys = rotate(
        (key_part * inverse).reshape(seq_count, kv_count, 2, head_dim), position
    ).astype(jnp.bfloat16)
    new_values = (value_part * inverse).astype(jnp.bfloat16).reshape(seq_count, kv_count, value_dim)
    group_size = HEADS // KV_HEADS
    kv_index = lax.axis_index("tp") * local_heads // group_size
    own_keys = lax.dynamic_slice_in_dim(key_cache, kv_index, 1, 1)[:, 0].reshape(
        seq_count, span_len, 2, head_dim
    )
    own_values = lax.dynamic_slice_in_dim(value_cache, kv_index, 1, 1)[:, 0]
    scale_root = math.sqrt(head_dim)
    scores = (
        jnp.einsum("bmcd,bpcd->bmcp", queries, own_keys, preferred_element_type=jnp.float32)
        / scale_root
    )
    places = lax.axis_index("kv") * span_len + jnp.arange(span_len, dtype=jnp.int32)
    visible = (places[None, :] < lengths[:, None])[:, None, None, :]
    scores = jnp.where(visible, scores, NEG)
    local_max = jnp.max(scores, axis=-1)
    weights = jnp.where(visible, jnp.exp(scores - local_max[..., None]), 0.0)
    local_sum = jnp.sum(weights, axis=-1)
    local_values = jnp.einsum(
        "bmcp,bpe->bmce",
        weights.astype(jnp.bfloat16),
        own_values,
        preferred_element_type=jnp.float32,
    )
    running_max, running_sum, weighted = joined(
        (local_max, local_sum, local_values), "kv", merge_parts
    )
    own_key = lax.dynamic_slice_in_dim(new_keys, kv_index, 1, 1)[:, 0].astype(jnp.float32)
    own_value = lax.dynamic_slice_in_dim(new_values, kv_index, 1, 1)[:, 0].astype(jnp.float32)
    own_scores = jnp.einsum("bmcd,bcd->bmc", queries.astype(jnp.float32), own_key) / scale_root
    joint = jnp.maximum(running_max, own_scores)
    past_factor = jnp.exp(running_max - joint)
    own_weight = jnp.exp(own_scores - joint)
    running_sum = running_sum * past_factor + own_weight
    weighted = (
        weighted * past_factor[..., None] + own_weight[..., None] * own_value[:, None, None, :]
    )
    outputs = weighted / running_sum[..., None]
    lambda_rows = mix_lambda[None, :, None]
    head_out = outputs[:, :, 0, :] - lambda_rows * outputs[:, :, 1, :]
    normed = (
        head_out
        * lax.rsqrt(jnp.mean(head_out * head_out, axis=-1, keepdims=True) + EPS)
        * head_gain.astype(jnp.float32)
    ).astype(jnp.bfloat16)
    partial_out = jnp.dot(
        normed.reshape(seq_count, local_heads * value_dim),
        out_weight,
        preferred_element_type=jnp.float32,
    ).astype(jnp.bfloat16)
    partial_out = lax.optimization_barrier(partial_out).astype(jnp.float32)
    mixed = lax.psum(partial_out.astype(jnp.bfloat16), "tp")
    return (mixed, new_keys.reshape(seq_count, kv_count, 2 * head_dim), new_values)


MESH = pl.DeviceIdType.MESH
CHUNKS = 4


def fused_kernel(
    dims,
    hidden_h,
    gain_h,
    lens_h,
    lam_h,
    head_gain_h,
    freq_h,
    expand_h,
    owner_seq_h,
    lane_pos_h,
    collect_h,
    query_w,
    key_w,
    value_w,
    key_c,
    value_c,
    out_w,
    mixed,
    new_keys,
    new_values,
    hidden,
    gain,
    lens,
    lam,
    head_gain,
    freq,
    expand,
    owner_seq,
    lane_pos,
    collect,
    qw_v,
    kw_v,
    vw_v,
    kc_v,
    vc_v,
    ow_v,
    scaled_v,
    q_v,
    qrows,
    limits,
    own_kv,
    vsend,
    vrecv,
    srecv,
    gain_rows,
    pad_v,
    nbuf,
    pbuf,
    in_sem,
    small_sem,
    vs_sem,
    vr_sem,
    ns_sem,
    nr_sem,
    ps_sem,
    pr_sem,
):
    n, tp, seqs, lh, kvc, span, head_dim, vd, group = dims
    spo = seqs // n
    ro = 2 * spo * lh
    half = spo * lh
    npair = n // 2
    width = 2 * head_dim
    me = lax.axis_index("kv")
    tpi = lax.axis_index("tp")
    par = lax.rem(me, 2)
    pair = lax.div(me, 2)
    kvh = lax.div(tpi * lh, group)
    d = hidden.shape[1]
    ck = d // CHUNKS

    small = []
    for i, (src, dst) in enumerate(
        (
            (hidden_h, hidden),
            (gain_h, gain),
            (lens_h, lens),
            (freq_h, freq),
            (owner_seq_h, owner_seq),
            (head_gain_h, head_gain),
            (lam_h, lam),
            (expand_h, expand),
            (lane_pos_h, lane_pos),
            (collect_h, collect),
        )
    ):
        cp = pltpu.make_async_copy(src, dst, small_sem.at[i])
        cp.start()
        small.append(cp)
    q_copies = []
    for i in range(CHUNKS):
        rows = pl.ds(i * ck, ck)
        cp = pltpu.make_async_copy(query_w.at[rows], qw_v.at[rows], in_sem.at[i])
        cp.start()
        q_copies.append(cp)
    kc_cp = pltpu.make_async_copy(key_c.at[:, kvh], kc_v, in_sem.at[CHUNKS])
    vc_cp = pltpu.make_async_copy(value_c.at[:, kvh], vc_v, in_sem.at[CHUNKS + 1])
    kw_cp = pltpu.make_async_copy(key_w, kw_v, in_sem.at[CHUNKS + 2])
    vw_cp = pltpu.make_async_copy(value_w, vw_v, in_sem.at[CHUNKS + 3])
    ow_cp = pltpu.make_async_copy(out_w, ow_v, in_sem.at[CHUNKS + 4])
    kc_cp.start()
    vc_cp.start()

    barrier = pltpu.get_barrier_semaphore()
    for k in range(1, n):
        pl.semaphore_signal(
            barrier, inc=1, device_id=(lax.rem(me + k, n), tpi), device_id_type=MESH
        )
    for k in range(1, tp):
        pl.semaphore_signal(
            barrier, inc=1, device_id=(me, lax.rem(tpi + k, tp)), device_id_type=MESH
        )

    for cp in small[:6]:
        cp.wait()
    inputs = hidden[...].astype(jnp.float32)
    inverse = lax.rsqrt(jnp.mean(inputs * inputs, axis=-1, keepdims=True) + EPS)
    scaled_v[...] = (inputs * gain[...].astype(jnp.float32)[None, :]).astype(jnp.bfloat16)
    lens_f = lens[...].astype(jnp.float32)
    rr = lax.broadcasted_iota(jnp.int32, (seqs, seqs), 0)
    cc = lax.broadcasted_iota(jnp.int32, (seqs, seqs), 1)
    lens_col = jnp.sum(jnp.where(rr == cc, lens_f, 0.0), axis=1, keepdims=True)
    angles = lens_col * freq[...]
    lane = lax.broadcasted_iota(jnp.int32, (seqs, width), 1)
    low = lax.rem(lane, head_dim) < head_dim // 2
    first = lane < head_dim
    cosine = jnp.cos(angles)
    sine = jnp.sin(angles)
    signed = jnp.where(low, -sine, sine)

    def turn(x):
        other = jnp.where(
            low,
            pltpu.roll(x, width - head_dim // 2, 1),
            pltpu.roll(x, head_dim // 2, 1),
        )
        return x * cosine + other * signed

    rel = jnp.clip(lens_col - (me * span).astype(jnp.float32), 0.0, float(span))
    rel = jnp.broadcast_to(rel, (seqs, width)).astype(jnp.bfloat16)
    limits[...] = jnp.dot(
        owner_seq[...], rel, preferred_element_type=jnp.float32
    ).reshape(n, ro, width)
    for b in range(spo):
        gain_rows[pl.ds(b * lh, lh), :] = head_gain[...].astype(jnp.float32)
    pad_v[...] = jnp.zeros_like(pad_v)

    acc = jnp.zeros((seqs, lh * width), jnp.float32)
    for i in range(CHUNKS):
        q_copies[i].wait()
        if i == CHUNKS - 1:
            kw_cp.start()
            vw_cp.start()
            ow_cp.start()
        acc = acc + jnp.dot(
            scaled_v[:, i * ck : (i + 1) * ck],
            qw_v[i * ck : (i + 1) * ck, :],
            preferred_element_type=jnp.float32,
        )
    for m in range(lh):
        t = turn(acc[:, m * width : (m + 1) * width] * inverse)
        q_v[pl.ds(m * seqs, seqs), :] = jnp.where(first, t, 0.0).astype(jnp.bfloat16)
        q_v[pl.ds((lh + m) * seqs, seqs), :] = jnp.where(first, 0.0, t).astype(jnp.bfloat16)
    for cp in small[6:]:
        cp.wait()
    qrows[...] = jnp.dot(
        expand[...], q_v[...], preferred_element_type=jnp.float32
    ).reshape(n, ro, width)

    scale = 1.0 / math.sqrt(head_dim)
    rid = lax.broadcasted_iota(jnp.int32, (ro, vd), 0)
    lid = lax.broadcasted_iota(jnp.int32, (ro, vd), 1)
    tail_row = lax.broadcasted_iota(jnp.int32, (8, vd), 0)
    at_max = lid == rid
    at_sum = lid == rid + vd // 2
    kc_cp.wait()
    vc_cp.wait()
    gs = 2 * spo
    order = sorted(range(1, npair), key=lambda k: -min(k, npair - k)) + [0]
    sends = []

    def send(k):
        gi = lax.rem(pair + k, npair)
        for j in range(2):
            if k == 0 and j == 0:
                continue
            t = 2 * gi + par + j * (1 - 2 * par)
            slot = 2 * k + j
            cp = pltpu.make_async_remote_copy(
                src_ref=vsend.at[t],
                dst_ref=vrecv.at[slot],
                send_sem=vs_sem.at[slot],
                recv_sem=vr_sem.at[slot],
                device_id=(t, tpi),
                device_id_type=MESH,
            )
            cp.start()
            sends.append(cp)

    def place(k):
        return lax.rem(pair + k, npair)

    batch = max(1, npair // 2)
    for start in range(0, npair, batch):
        ks = order[start : start + batch]
        scores = []
        for k in ks:
            gi = place(k)
            q = qrows[pl.ds(2 * gi, 2)].reshape(2 * ro, width).astype(jnp.bfloat16)
            keys = kc_v[pl.ds(gi * gs, gs)].reshape(gs * span, width)
            scores.append(
                lax.dot_general(
                    q, keys, (((1,), (1,)), ((), ())), preferred_element_type=jnp.float32
                )
            )
        soft = []
        for k, s in zip(ks, scores):
            lim = limits[pl.ds(2 * place(k), 2)].reshape(2 * ro, width)
            visible = lane_pos[...] < lim[:, :1]
            s = jnp.where(visible, s * scale, NEG)
            mx = jnp.max(s, axis=1, keepdims=True)
            w = jnp.where(visible, jnp.exp(s - mx), 0.0)
            soft.append((mx, jnp.sum(w, axis=1, keepdims=True), w.astype(jnp.bfloat16)))
        values = []
        for k, (_, _, w) in zip(ks, soft):
            vals = vc_v[pl.ds(place(k) * gs, gs)].reshape(gs * span, vd)
            values.append(jnp.dot(w, vals, preferred_element_type=jnp.float32))
        for k, (mx, sm, _), o in zip(ks, soft, values):
            gi = place(k)
            for j in range(2):
                rows = slice(j * ro, (j + 1) * ro)
                stat = jnp.where(at_max, mx[rows], jnp.where(at_sum, sm[rows], 0.0))
                stat = jnp.sum(stat, axis=0, keepdims=True)
                high = stat.astype(jnp.bfloat16).astype(jnp.float32)
                middle = (stat - high).astype(jnp.bfloat16).astype(jnp.float32)
                lowest = stat - high - middle
                tail = jnp.where(
                    tail_row == 0,
                    high,
                    jnp.where(tail_row == 1, middle, jnp.where(tail_row == 2, lowest, 0.0)),
                )
                both = jnp.concatenate([o[rows], tail], axis=0)
                vsend[2 * gi + j] = both.astype(jnp.bfloat16)
        if start == 0:
            pl.semaphore_wait(barrier, n - 1 + tp - 1)
        for k in ks:
            send(k)

    kw_cp.wait()
    kp = jnp.dot(scaled_v[...], kw_v[...], preferred_element_type=jnp.float32) * inverse
    vw_cp.wait()
    vp = jnp.dot(scaled_v[...], vw_v[...], preferred_element_type=jnp.float32) * inverse
    for g in range(kvc):
        nk = turn(kp[:, g * width : (g + 1) * width]).astype(jnp.bfloat16)
        nv = vp[:, g * vd : (g + 1) * vd].astype(jnp.bfloat16)
        new_keys[:, g, :] = nk
        new_values[:, g, :] = nv
        own_kv[0, g] = nk
        own_kv[1, g] = nv
    sr = lax.broadcasted_iota(jnp.int32, (ro, seqs), 0)
    sc = lax.broadcasted_iota(jnp.int32, (ro, seqs), 1)
    pick = (sc == me * spo + lax.div(lax.rem(sr, half), lh)).astype(jnp.float32)
    pick = pick.astype(jnp.bfloat16)
    kx = jnp.dot(pick, own_kv[0, kvh], preferred_element_type=jnp.float32)
    vx = jnp.dot(pick, own_kv[1, kvh], preferred_element_type=jnp.float32)
    own = jnp.sum(qrows[me] * kx, axis=1, keepdims=True) * scale
    lam_row = lax.broadcasted_iota(jnp.int32, (half, lh), 0)
    lam_col = lax.broadcasted_iota(jnp.int32, (half, lh), 1)
    mix = jnp.sum(
        jnp.where(lax.rem(lam_row, lh) == lam_col, lam[...], 0.0), axis=1, keepdims=True
    )

    vrecv[0] = vsend[me]
    for cp in sends:
        cp.wait()
    for s in range(n):
        tail = vrecv[s].astype(jnp.float32)[ro:]
        srecv[s : s + 1, :] = tail[0:1] + tail[1:2] + tail[2:3]
    stats = jnp.transpose(srecv[...])
    maxima = stats[:ro]
    sums = stats[vd // 2 : vd // 2 + ro]
    top = jnp.maximum(jnp.max(maxima, axis=1, keepdims=True), own)
    factor = jnp.exp(maxima - top)
    own_w = jnp.exp(own - top)
    total = jnp.sum(factor * sums, axis=1, keepdims=True) + own_w
    weighted = own_w * vx
    for s in range(n):
        weighted = weighted + factor[:, s : s + 1] * vrecv[s].astype(jnp.float32)[:ro]
    outputs = weighted / total
    head_out = outputs[:half] - mix * outputs[half:]
    norm = lax.rsqrt(jnp.mean(head_out * head_out, axis=-1, keepdims=True) + EPS)
    pad_v[pl.ds(0, half), :] = head_out * norm * gain_rows[...]
    nbuf[me] = pad_v[...].astype(jnp.bfloat16)
    sends = []
    for k in range(1, n):
        cp = pltpu.make_async_remote_copy(
            src_ref=nbuf.at[me],
            dst_ref=nbuf.at[me],
            send_sem=ns_sem.at[k],
            recv_sem=nr_sem.at[k],
            device_id=(lax.rem(me + k, n), tpi),
            device_id_type=MESH,
        )
        cp.start()
        sends.append(cp)
    ow_cp.wait()
    for cp in sends:
        cp.wait()
    rows_in = nbuf[...].reshape(nbuf.shape[0] * nbuf.shape[1], vd)
    normed = jnp.dot(collect[...], rows_in, preferred_element_type=jnp.float32).astype(
        jnp.bfloat16
    )
    part = jnp.zeros((seqs, ow_v.shape[0]), jnp.float32)
    for m in range(lh):
        part = part + lax.dot_general(
            normed[m * seqs : (m + 1) * seqs],
            ow_v[:, m * vd : (m + 1) * vd],
            (((1,), (1,)), ((), ())),
            preferred_element_type=jnp.float32,
        )
    pbuf[0] = part.astype(jnp.bfloat16)
    sends = []
    for k in range(1, tp):
        cp = pltpu.make_async_remote_copy(
            src_ref=pbuf.at[0],
            dst_ref=pbuf.at[k],
            send_sem=ps_sem.at[k],
            recv_sem=pr_sem.at[k],
            device_id=(me, lax.rem(tpi + k, tp)),
            device_id_type=MESH,
        )
        cp.start()
        sends.append(cp)
    for cp in sends:
        cp.wait()
    summed = pbuf[0].astype(jnp.float32)
    for k in range(1, tp):
        summed = summed + pbuf[k].astype(jnp.float32)
    mixed[...] = summed.astype(jnp.bfloat16)


def write_out(*refs):
    copies = [
        pltpu.make_async_copy(refs[i], refs[3 + i], refs[6].at[i]) for i in range(3)
    ]
    for cp in copies:
        cp.start()
    for cp in copies:
        cp.wait()


def tables(n, seqs, lh, span, head_dim, pad):
    spo = seqs // n
    half = spo * lh
    ro = 2 * half
    row = np.arange(n * ro)
    owner, rem = row // ro, row % ro
    pair_map, b, m = rem // half, owner * spo + (rem % half) // lh, rem % lh
    expand = np.zeros((n * ro, 2 * lh * seqs), np.float32)
    expand[row, (pair_map * lh + m) * seqs + b] = 1.0
    owner_seq = np.zeros((n * ro, seqs), np.float32)
    owner_seq[row, b] = 1.0
    lanes = np.arange(2 * spo * span)
    lane_pos = np.where(
        (b[: 2 * ro])[:, None] == (lanes // span)[None, :], lanes % span, 1 << 20
    ).astype(np.float32)
    collect = np.zeros((lh * seqs, n * pad), np.float32)
    for h in range(lh):
        for s in range(seqs):
            collect[h * seqs + s, (s // spo) * pad + (s % spo) * lh + h] = 1.0
    half_dim = head_dim // 2
    freq = THETA ** (-np.arange(half_dim) * 2.0 / head_dim)
    freq = np.tile(freq, 4)[None, :].astype(np.float32)
    bf = lambda a: jnp.asarray(a, jnp.bfloat16)
    return jnp.asarray(freq), bf(expand), bf(owner_seq), jnp.asarray(lane_pos), bf(collect)


def fused_device(mesh_shape, *args):
    (
        hidden_in,
        in_gain,
        query_weight,
        key_weight,
        value_weight,
        key_cache,
        value_cache,
        lengths,
        mix_lambda,
        head_gain,
        out_weight,
    ) = args
    n, tp = mesh_shape
    seqs, d = hidden_in.shape
    lh = mix_lambda.shape[0]
    head_dim = query_weight.shape[1] // (2 * lh)
    width = 2 * head_dim
    _, kvc, span, vd = value_cache.shape
    spo = seqs // n
    ro = 2 * spo * lh
    pad = -(-(ro // 2) // 16) * 16
    dims = (n, tp, seqs, lh, kvc, span, head_dim, vd, HEADS // KV_HEADS)
    bf, f32 = jnp.bfloat16, jnp.float32
    vmem = pl.BlockSpec(memory_space=pltpu.VMEM)
    hbm = pl.BlockSpec(memory_space=pltpu.HBM)
    dma = pltpu.SemaphoreType.DMA
    consts = tables(n, seqs, lh, span, head_dim, pad)
    smalls = (
        hidden_in,
        in_gain,
        lengths.reshape(1, seqs),
        mix_lambda.reshape(1, lh),
        head_gain,
        *consts,
    )
    out_weight = jnp.transpose(out_weight)
    features = out_weight.shape[0]
    results = ((seqs, features), (seqs, kvc, width), (seqs, kvc, vd))
    held = pl.pallas_call(
        functools.partial(fused_kernel, dims),
        name="fused",
        out_shape=tuple(pltpu.VMEM(shape, bf) for shape in results),
        in_specs=[hbm] * 16,
        out_specs=(vmem, vmem, vmem),
        scratch_shapes=[pltpu.VMEM(a.shape, a.dtype) for a in smalls]
        + [
            pltpu.VMEM(query_weight.shape, bf),
            pltpu.VMEM(key_weight.shape, bf),
            pltpu.VMEM(value_weight.shape, bf),
            pltpu.VMEM((seqs, span, width), bf),
            pltpu.VMEM((seqs, span, vd), bf),
            pltpu.VMEM(out_weight.shape, bf),
            pltpu.VMEM((seqs, d), bf),
            pltpu.VMEM((2 * lh * seqs, width), bf),
            pltpu.VMEM((n, ro, width), f32),
            pltpu.VMEM((n, ro, width), f32),
            pltpu.VMEM((2, kvc, seqs, width), bf),
            pltpu.VMEM((n, ro + 8, vd), bf),
            pltpu.VMEM((n, ro + 8, vd), bf),
            pltpu.VMEM((n, vd), f32),
            pltpu.VMEM((ro // 2, vd), f32),
            pltpu.VMEM((pad, vd), f32),
            pltpu.VMEM((n, pad, vd), bf),
            pltpu.VMEM((tp, seqs, features), bf),
            dma((CHUNKS + 5,)),
            dma((10,)),
        ]
        + [dma((n,))] * 4
        + [dma((tp,))] * 2,
        compiler_params=pltpu.CompilerParams(
            collective_id=0, has_side_effects=True, vmem_limit_bytes=32 * 1024 * 1024
        ),
    )(
        *(
            pltpu.with_memory_space_constraint(a, pltpu.HBM)
            for a in (
                *smalls,
                query_weight,
                key_weight,
                value_weight,
                key_cache,
                value_cache,
                out_weight,
            )
        )
    )
    return pl.pallas_call(
        write_out,
        name="write_out",
        out_shape=tuple(jax.ShapeDtypeStruct(shape, bf) for shape in results),
        in_specs=[vmem] * 3,
        out_specs=(hbm,) * 3,
        scratch_shapes=[dma((3,))],
    )(*(pltpu.with_memory_space_constraint(a, pltpu.VMEM) for a in held))


def choose(mesh_shape, *args):
    n, tp = mesh_shape
    seqs = args[0].shape[0]
    lh = args[8].shape[0]
    head_dim = args[2].shape[1] // (2 * lh)
    span = args[5].shape[2]
    vd = args[6].shape[3]
    fits = (
        n % 2 == 0
        and seqs % n == 0
        and (2 * (seqs // n) * lh) % 8 == 0
        and 2 * (seqs // n) * lh <= vd // 2
        and 2 * head_dim == vd == 128
        and span <= 256
        and (HEADS // KV_HEADS) % lh == 0
    )
    if fits:
        return fused_device(mesh_shape, *args)
    return per_device(*args)


def solution(mesh):
    return jax.shard_map(
        functools.partial(choose, (mesh.shape["kv"], mesh.shape["tp"])),
        mesh=mesh,
        in_specs=(
            P(),
            P(),
            P(None, "tp"),
            P(),
            P(),
            P(None, None, "kv", None),
            P(None, None, "kv", None),
            P(),
            P("tp"),
            P("tp", None),
            P("tp", "kv"),
        ),
        out_specs=(P(None, "kv"), P(), P()),
        check_vma=False,
    )
```
